32 devices in a mesh: ep: 4 (over z), tp: 8 (over y, x, core).
Axes of the slice: x: 2, y: 2, z: 4, core: 2. Of those that a mesh axis runs over, the one named last changes fastest.
Arguments:
- tokens: bfloat16 [672, 2048], P('ep', 'tp'), may hold values from -540 to 540
- norm_gain: float32 [2048], P('tp'), may hold values from 0.1 to 1.9
- chosen: int32 [4, 504], P('ep'), may hold values from 0 to 671, as said below
- affinity: float32 [4, 504], P('ep'), may hold values from 0.1 to 1
- w_gate: bfloat16 [4, 2048, 8192], P('ep', None, 'tp'), may hold values from -0.125 to 0.125
- w_up: bfloat16 [4, 2048, 8192], P('ep', None, 'tp'), may hold values from -0.125 to 0.125
- w_down: bfloat16 [4, 8192, 2048], P('ep', 'tp'), may hold values from -0.0625 to 0.0625
Outputs:
- expert_mix: bfloat16 [672, 2048], P('ep', 'tp')
The draws below stay inside these ranges and needn't reach their ends.
Inputs may be any that keep to these rules, and one draw needn't show every extreme that they name: `chosen`: each expert's 504 token numbers are distinct. Among one expert's choices at most 168 are tokens of one index of ep, and that bound is reached in every draw.
All inputs are finite; a program needn't handle non-finite values.
Results may differ from the reference program's by a relative error of at most 0.025.
Values may be sent and summed in bfloat16 or wider, within the bound.
A program may use at most 64 MiB of HBM per device.

```python
import math
import jax
import jax.numpy as jnp
from jax import lax

D = 2048
FF = 8192
TOK_DEV = 168
TOKENS = 672
EXPERTS = 4
CHOSEN = 504
MOST = 168
N_TP = 8


def draw_tokens(key, part):
    key_noise, key_cols, key_rows = jax.random.split(key, 3)
    col_scale = 6.0 ** (jnp.arange(D, dtype=jnp.float32) / (D - 1))
    col_scale = col_scale * jax.random.uniform(key_cols, (D,), jnp.float32, 0.5, 1.5)
    row_scale = jnp.exp(jax.random.uniform(key_rows, (TOKENS, 1), jnp.float32, 0.0, math.log(10.0)))
    noise = jnp.clip(jax.random.normal(key_noise, (TOKENS, D), jnp.float32), -6.0, 6.0)
    return (noise * col_scale[None, :] * row_scale).astype(jnp.bfloat16)


def draw_chosen(key, part):

    def pick_expert(expert):
        expert_key = jax.random.fold_in(key, expert)
        key_raw, key_full = jax.random.split(expert_key, 2)
        raw_score = jax.random.randint(key_raw, (EXPERTS, TOK_DEV), 0, 32768)
        local_id = jnp.arange(TOK_DEV, dtype=jnp.int32)[None, :]
        source = jnp.arange(EXPERTS, dtype=jnp.int32)[:, None]
        global_id = source * TOK_DEV + local_id
        keyed_score = raw_score * TOK_DEV + local_id
        ranked = jnp.argsort(jnp.argsort(-keyed_score, axis=1), axis=1)
        allowed = ranked < MOST
        full_source = jax.random.randint(key_full, (), 0, EXPERTS)
        before = (expert + EXPERTS - 1) % EXPERTS
        across = (expert + EXPERTS // 2) % EXPERTS
        extra_score = jnp.where(source == full_source, 2, 0)
        extra_score = extra_score + jnp.where(((source == before) | (source == across)) & (ranked == 0), 4, 0)
        priority = allowed.astype(jnp.int32) * (extra_score + 1) * (1 << 27) + raw_score * TOKENS + global_id
        return lax.top_k(priority.reshape(-1), CHOSEN)[1].astype(jnp.int32)
    from_experts = jax.vmap(pick_expert)(jnp.arange(EXPERTS, dtype=jnp.int32))
    return from_experts.astype(jnp.int32)


def levels(rng, dims, cuts, least, high):
    factor_of, own = 1.0, jax.random.fold_in(rng, 6)
    for position, shards_of in cuts:
        draws = jnp.exp(jax.random.uniform(jax.random.fold_in(own, position), (shards_of,), jnp.float32, least / len(cuts), high / len(cuts)))
        factor_of = factor_of * jnp.repeat(draws, dims[position] // shards_of).reshape([-1 if axis == position else 1 for axis in range(len(dims))])
    return factor_of


def bell_draw(rng, shape, deviation, reach, shards=(), held_as=jnp.bfloat16):
    drawn = deviation * jax.random.normal(rng, shape, jnp.float32)
    if shards:
        drawn = drawn * levels(rng, shape, shards, -0.22, 0.18)
    return jnp.clip(drawn, -reach, reach).astype(held_as)


def setup_inputs(seed: int = 0) -> dict:
    arg_keys = jax.random.split(jax.random.key(seed), 8)
    return {
        "tokens": draw_tokens(jax.random.fold_in(arg_keys[7], 71), 0),
        "norm_gain": jnp.clip(1.0 + 0.18 * jax.random.normal(arg_keys[1], (D,), jnp.float32), 0.1, 1.9),
        "chosen": draw_chosen(jax.random.fold_in(arg_keys[7], 71), 0),
        "affinity": jnp.clip(jnp.exp(math.log(1.0) - 2.3025851 * jax.random.uniform(arg_keys[3], (EXPERTS, CHOSEN), jnp.float32) ** levels(arg_keys[3], (EXPERTS, CHOSEN), ((0, 4),), -0.2, 0.2)), 0.1, 1.0),
        "w_gate": bell_draw(arg_keys[4], (EXPERTS, D, FF), D ** -0.5, 0.125, ((0, 4), (2, 8))),
        "w_up": bell_draw(arg_keys[5], (EXPERTS, D, FF), D ** -0.5, 0.125, ((0, 4), (2, 8))),
        "w_down": bell_draw(arg_keys[6], (EXPERTS, FF, D), FF ** -0.5, 0.0625, ((0, 4), (1, 8))),
    }


EPS = 1e-06

def reference(tokens, norm_gain, chosen, affinity, w_gate, w_up, w_down):
    floats = tokens.astype(jnp.float32)
    mean_square = lax.optimization_barrier(jnp.mean(floats * floats, axis=1))
    normed = (floats * lax.rsqrt(mean_square + EPS)[:, None] * norm_gain[None, :]).astype(jnp.bfloat16)

    def single(packed):
        index_row, weight_row, gate_weights, up_weights, down_weights = packed
        picked = normed[index_row]
        gate = jnp.dot(picked, gate_weights, preferred_element_type=jnp.float32)
        upward = jnp.dot(picked, up_weights, preferred_element_type=jnp.float32)
        hidden = (jax.nn.silu(gate) * upward).astype(jnp.bfloat16)
        blocks = hidden.reshape(hidden.shape[0], N_TP, FF // N_TP).astype(jnp.float32)
        down_blocks = down_weights.reshape(N_TP, FF // N_TP, D).astype(jnp.float32)
        partial_value = jnp.einsum('cnf,nfd->ncd', blocks, down_blocks).astype(jnp.bfloat16)
        partial_value = lax.optimization_barrier(partial_value)
        summed = lax.optimization_barrier(jnp.sum(partial_value.astype(jnp.float32), axis=0))
        return (summed * weight_row[:, None]).astype(jnp.bfloat16)
    outputs = lax.map(single, (chosen, affinity, w_gate, w_up, w_down))
    total = jnp.zeros((TOKENS, D), jnp.float32)
    total = total.at[chosen.reshape(-1)].add(outputs.reshape(-1, D).astype(jnp.float32))
    return total.astype(jnp.bfloat16)
```

```python
import functools

import jax
import jax.numpy as jnp
from jax import lax
from jax.experimental import pallas as pl
from jax.experimental.pallas import tpu as pltpu
from jax.sharding import PartitionSpec as P

MESH = pl.DeviceIdType.MESH
VMEM_BYTES = 67_043_328
LANES = 128
CHUNKS = 2


def kernel(
    ep, tp, chunks,
    tok, gain, chosen, aff, wg_hbm, wu_hbm, wd_hbm,
    out,
    wg, wu, wd, full, normed, hidden, part, got1, got2, own, weighted,
    near, back, got_back, chosen_row, aff_row, chosen_col, aff_col,
    w_sem, z_send, z_recv, ag_send, ag_recv,
    r1_send, r1_recv, r2_send, r2_recv, b_send, b_recv,
):
    me = lax.axis_index("ep")
    t = lax.axis_index("tp")
    tok_dev, width = tok.shape
    rows, d = full.shape
    count = chosen.shape[1]
    size = rows // chunks
    ff = wg.shape[1]
    f32, bf16 = jnp.float32, jnp.bfloat16

    def flip(m):
        index, bit = t, 1
        while bit <= m:
            if m & bit:
                index = index + bit - 2 * bit * ((t // bit) % 2)
            bit *= 2
        return index

    def cols(m):
        return pl.ds(pl.multiple_of(flip(m) * width, LANES), width)

    def remote(src, dst, send, recv, ep_to, tp_to):
        return pltpu.make_async_remote_copy(
            src_ref=src, dst_ref=dst, send_sem=send, recv_sem=recv,
            device_id=(ep_to, tp_to), device_id_type=MESH,
        )

    evens = list(range(2, tp, 2))
    weights = [
        pltpu.make_async_copy(h.at[0], v, w_sem.at[i])
        for i, (h, v) in enumerate(((wg_hbm, wg), (wu_hbm, wu), (wd_hbm, wd)))
    ]
    for copy in weights:
        copy.start()

    barrier = pltpu.get_barrier_semaphore()
    for m in [1] + evens:
        pl.semaphore_signal(barrier, inc=1, device_id=(me, flip(m)), device_id_type=MESH)
    for k in range(1, ep):
        pl.semaphore_signal(
            barrier, inc=1, device_id=(lax.rem(me + k, ep), t), device_id_type=MESH
        )
    pl.semaphore_wait(barrier, len(evens) + ep)

    def z_copy(k):
        return remote(
            tok, near.at[k], z_send.at[k], z_recv.at[k], lax.rem(me + k, ep), t
        )

    for k in range(1, ep):
        z_copy(k).start()

    chosen_row[...] = jnp.full(chosen_row.shape, -1.0, f32)
    aff_row[...] = jnp.zeros(aff_row.shape, f32)
    chosen_row[:, :count] = chosen[...].astype(f32)
    aff_row[:, :count] = aff[...]
    diagonal = lax.broadcasted_iota(jnp.int32, (rows, rows), 0) == lax.broadcasted_iota(
        jnp.int32, (rows, rows), 1
    )
    chosen_col[...] = jnp.sum(jnp.where(diagonal, chosen_row[...], 0.0), axis=1, keepdims=True)
    aff_col[...] = jnp.sum(jnp.where(diagonal, aff_row[...], 0.0), axis=1, keepdims=True)

    g = gain[...]
    g0 = g.astype(bf16).astype(f32)
    g1 = (g - g0).astype(bf16).astype(f32)
    g2 = g - g0 - g1

    order = list(range(chunks))[::-1]

    def span(c):
        return pl.ds(c * size, size)

    def ag_copy(c, m, via):
        block = full.at[span(c), cols(via)]
        return remote(
            block, block, ag_send.at[c, m], ag_recv.at[c, m], me, flip(m) if via == 0 else flip(1)
        )

    def ag_wait(c, m):
        block = full.at[span(c), cols(m)]
        remote(block, block, ag_send.at[c, m], ag_recv.at[c, m], me, flip(m)).wait_recv()

    for k in range(1, ep):
        z_copy(k).wait_recv()
    lane_token = lax.broadcasted_iota(jnp.int32, (size, tok_dev), 1)
    for c in order:
        total = None
        for k in range(ep):
            source = lax.rem(me + ep - k, ep)
            hot = (chosen_col[span(c), :] == (lane_token + source * tok_dev).astype(f32)).astype(f32)
            block = tok[...] if k == 0 else near[k]
            product = jnp.dot(hot.astype(bf16), block, preferred_element_type=f32)
            total = product if total is None else total + product
        if c == order[0]:
            row = lax.broadcasted_iota(jnp.int32, (size, width), 0)
            total = jnp.where(row == size - 3, g0, total)
            total = jnp.where(row == size - 2, g1, total)
            total = jnp.where(row == size - 1, g2, total)
        full[span(c), cols(0)] = total.astype(bf16)
        for m in evens + [1]:
            ag_copy(c, m, 0).start()

    def forward(c):
        for m in evens:
            ag_wait(c, m)
            ag_copy(c, m + 1, m).start()

    tile = min(ff, 256)
    forward(order[0])
    gain_all = None
    for position, c in enumerate(order):
        for m in range(1, tp, 2):
            ag_wait(c, m)
        if gain_all is None:
            last = full[pl.ds(rows - 16, 16), :].astype(f32)
            gain_all = (last[15:16, :] + last[14:15, :]) + last[13:14, :]
        floats = full[span(c), :].astype(f32)
        mean_square = jnp.sum(floats * floats, axis=1, keepdims=True) / d
        normed[...] = (floats * lax.rsqrt(mean_square + EPS) * gain_all).astype(bf16)
        if position == 0:
            weights[0].wait()
            weights[1].wait()

        @pl.loop(0, ff // tile)
        def _(j):
            units = pl.ds(pl.multiple_of(j * tile, LANES), tile)
            gate = jnp.dot(normed[...], wg[:, units], preferred_element_type=f32)
            upward = jnp.dot(normed[...], wu[:, units], preferred_element_type=f32)
            hidden[:, units] = (gate / (1.0 + jnp.exp(-gate)) * upward).astype(bf16)

        if position + 1 < chunks:
            forward(order[position + 1])
        if position == 0:
            weights[2].wait()

        def down(m):
            return jnp.dot(hidden[...], wd[:, cols(m)], preferred_element_type=f32)

        for m in [e + 1 for e in evens] + [1]:
            part[c, m] = down(m).astype(bf16)
            remote(
                part.at[c, m], got1.at[c, m - 1], r1_send.at[c, m], r1_recv.at[c, m - 1],
                me, flip(1),
            ).start()
        for m in evens + [0]:
            mine = down(m)
            remote(
                part.at[c, m + 1], got1.at[c, m], r1_send.at[c, m + 1], r1_recv.at[c, m],
                me, flip(1),
            ).wait_recv()
            mine = mine + got1[c, m].astype(f32)
            if m:
                part[c, m] = mine.astype(bf16)
                remote(
                    part.at[c, m], got2.at[c, m], r2_send.at[c, m], r2_recv.at[c, m], me, flip(m)
                ).start()
            else:
                own[span(c), :] = mine

    for c in order:
        total = own[span(c), :]
        for m in evens:
            remote(
                part.at[c, m], got2.at[c, m], r2_send.at[c, m], r2_recv.at[c, m], me, flip(m)
            ).wait_recv()
            total = total + got2[c, m].astype(f32)
        weighted[span(c), :] = (total * aff_col[span(c), :]).astype(bf16)

    sub_token = lax.broadcasted_iota(jnp.int32, (tok_dev, rows), 0)

    def at_tokens(owner):
        hot = (chosen_row[...] == (sub_token + owner * tok_dev).astype(f32)).astype(f32)
        return jnp.dot(hot.astype(bf16), weighted[...], preferred_element_type=f32)

    def back_copy(k):
        return remote(
            back.at[k], got_back.at[k], b_send.at[k], b_recv.at[k], lax.rem(me + k, ep), t
        )

    for k in range(1, ep):
        back[k] = at_tokens(lax.rem(me + k, ep)).astype(bf16)
        back_copy(k).start()
    mix = at_tokens(me)
    for k in range(1, ep):
        back_copy(k).wait_recv()
        mix = mix + got_back[k].astype(f32)
    out[...] = mix.astype(bf16)

    for k in range(1, ep):
        z_copy(k).wait_send()
        back_copy(k).wait_send()
    for c in order:
        for m in evens + [1]:
            ag_copy(c, m, 0).wait_send()
        for m in evens:
            ag_copy(c, m + 1, m).wait_send()
            remote(
                part.at[c, m], got2.at[c, m], r2_send.at[c, m], r2_recv.at[c, m], me, flip(m)
            ).wait_send()
        for m in range(1, tp, 2):
            remote(
                part.at[c, m], got1.at[c, m - 1], r1_send.at[c, m], r1_recv.at[c, m - 1],
                me, flip(1),
            ).wait_send()


def fused(ep, tp, tokens, norm_gain, chosen, affinity, w_gate, w_up, w_down):
    tok_dev, width = tokens.shape
    d, ff = w_gate.shape[1:]
    count = chosen.shape[1]
    step = 16 * CHUNKS
    rows = -(-(count + 3) // step) * step
    size = rows // CHUNKS
    f32, bf16 = jnp.float32, jnp.bfloat16
    vmem = pl.BlockSpec(memory_space=pltpu.VMEM)
    hbm = pl.BlockSpec(memory_space=pl.ANY)
    dma = pltpu.SemaphoreType.DMA
    return pl.pallas_call(
        functools.partial(kernel, ep, tp, CHUNKS),
        out_shape=jax.ShapeDtypeStruct((tok_dev, width), bf16),
        in_specs=[vmem] * 4 + [hbm] * 3,
        out_specs=vmem,
        scratch_shapes=[
            pltpu.VMEM((d, ff), bf16),
            pltpu.VMEM((d, ff), bf16),
            pltpu.VMEM((ff, d), bf16),
            pltpu.VMEM((rows, d), bf16),
            pltpu.VMEM((size, d), bf16),
            pltpu.VMEM((size, ff), bf16),
            pltpu.VMEM((CHUNKS, tp, size, width), bf16),
            pltpu.VMEM((CHUNKS, tp, size, width), bf16),
            pltpu.VMEM((CHUNKS, tp, size, width), bf16),
            pltpu.VMEM((rows, width), f32),
            pltpu.VMEM((rows, width), bf16),
            pltpu.VMEM((ep, tok_dev, width), bf16),
            pltpu.VMEM((ep, tok_dev, width), bf16),
            pltpu.VMEM((ep, tok_dev, width), bf16),
            pltpu.VMEM((1, rows), f32),
            pltpu.VMEM((1, rows), f32),
            pltpu.VMEM((rows, 1), f32),
            pltpu.VMEM((rows, 1), f32),
            dma((3,)),
            dma((ep,)),
            dma((ep,)),
            dma((CHUNKS, tp)),
            dma((CHUNKS, tp)),
            dma((CHUNKS, tp)),
            dma((CHUNKS, tp)),
            dma((CHUNKS, tp)),
            dma((CHUNKS, tp)),
            dma((ep,)),
            dma((ep,)),
        ],
        compiler_params=pltpu.CompilerParams(
            collective_id=0, has_side_effects=True, vmem_limit_bytes=VMEM_BYTES
        ),
    )(tokens, norm_gain[None, :], chosen, affinity, w_gate, w_up, w_down)


EPS = 1e-06


def plain(tokens, norm_gain, chosen, affinity, w_gate, w_up, w_down):
    tok_dev, width_part = tokens.shape
    ep_count = lax.axis_size("ep")
    floats = tokens.astype(jnp.float32)
    square_sum = lax.psum(jnp.sum(floats * floats, axis=1), "tp")
    normed = (floats * lax.rsqrt(square_sum / w_gate.shape[1] + EPS)[:, None] * norm_gain[None, :]).astype(
        jnp.bfloat16
    )
    own_choice = chosen[0]
    chosen_count = own_choice.shape[0]
    bound_rows = min(tok_dev, 2 * chosen_count // ep_count)
    slot_ids = jnp.arange(bound_rows, dtype=jnp.int32)
    positions = jnp.arange(chosen_count, dtype=jnp.int32)
    every_token = lax.all_gather(normed, "ep", axis=0, tiled=True)
    picked = every_token[own_choice]
    piece = lax.all_gather(picked, "tp", axis=1, tiled=True)
    gate_rows = w_gate[0]
    up_rows = w_up[0]
    gate = jnp.dot(piece, gate_rows, preferred_element_type=jnp.float32)
    upward = jnp.dot(piece, up_rows, preferred_element_type=jnp.float32)
    hidden = (jax.nn.silu(gate) * upward).astype(jnp.bfloat16)
    columns = w_down[0]
    summed = lax.psum_scatter(
        lax.dot_general(
            columns, hidden, (((0,), (1,)), ((), ())), preferred_element_type=jnp.float32
        ).astype(jnp.bfloat16),
        "tp",
        scatter_dimension=0,
        tiled=True,
    ).astype(jnp.float32)
    weighted = (summed * affinity[0][None, :]).astype(jnp.bfloat16).T
    owner = own_choice // tok_dev
    owner_local = own_choice - owner * tok_dev
    owner_hot = owner[:, None] == jnp.arange(ep_count, dtype=jnp.int32)[None, :]
    running = jnp.cumsum(owner_hot.astype(jnp.int32), axis=0)
    place = jnp.sum(jnp.where(owner_hot, running, 0), axis=1) - 1
    back_match = owner_hot.T[:, None, :] & (place[None, None, :] == slot_ids[None, :, None])
    back_filled = jnp.any(back_match, axis=2)
    back_pick = jnp.sum(jnp.where(back_match, positions[None, None, :], 0), axis=2)
    back_rows = jnp.where(back_filled[..., None], weighted[back_pick], jnp.zeros((), jnp.bfloat16))
    back_token = jnp.where(back_filled, owner_local[back_pick], tok_dev)
    got_back, got_token = (
        lax.all_to_all(back_rows, "ep", split_axis=0, concat_axis=0, tiled=True),
        lax.all_to_all(back_token, "ep", split_axis=0, concat_axis=0, tiled=True),
    )
    total = jnp.zeros((tok_dev, width_part), jnp.float32)
    total = total.at[got_token.reshape(-1)].add(
        got_back.reshape(-1, width_part).astype(jnp.float32), mode="drop"
    )
    return total.astype(jnp.bfloat16)


def solution(mesh):
    ep, tp = mesh.shape["ep"], mesh.shape["tp"]

    def local(tokens, *rest):
        whole_lanes = tokens.shape[1] % LANES == 0 and rest[3].shape[2] % LANES == 0
        if whole_lanes and tp >= 4 and tp & (tp - 1) == 0:
            return fused(ep, tp, tokens, *rest)
        return plain(tokens, *rest)

    in_specs = (
        P("ep", "tp"),
        P("tp"),
        P("ep", None),
        P("ep", None),
        P("ep", None, "tp"),
        P("ep", None, "tp"),
        P("ep", "tp", None),
    )
    out_specs = P("ep", "tp")
    return jax.shard_map(local, mesh=mesh, in_specs=in_specs, out_specs=out_specs, check_vma=False)
```

```python
import functools

import jax
import jax.numpy as jnp
from jax import lax
from jax.experimental import pallas as pl
from jax.experimental.pallas import tpu as pltpu
from jax.sharding import PartitionSpec as P

MESH = pl.DeviceIdType.MESH
VMEM_BYTES = 67_043_328
LANES = 128
CHUNKS = 2
LAG = 1


def kernel(
    ep, tp, chunks,
    tok, gain, chosen, aff, wg_hbm, wu_hbm, wd_hbm,
    out,
    wg, wu, wd, full, normed, hidden, part, got1, got2, own, weighted,
    near, back, got_back, chosen_row, aff_row, aff_token, slot_row, slot_col,
    aff_col, gain_all, keep, w_sem, g_send, g_recv, z_send, z_recv, ag_send, ag_recv,
    r1_send, r1_recv, r2_send, r2_recv, b_send, b_recv,
):
    me = lax.axis_index("ep")
    t = lax.axis_index("tp")
    tok_dev, width = tok.shape
    rows = full.shape[1]
    d = wg.shape[0]
    count = chosen.shape[1]
    size = rows // chunks
    ff = wg.shape[1]
    f32, bf16 = jnp.float32, jnp.bfloat16

    def flip(m):
        index, bit = t, 1
        while bit <= m:
            if m & bit:
                index = index + bit - 2 * bit * ((t // bit) % 2)
            bit *= 2
        return index

    def cols(m):
        return pl.ds(pl.multiple_of(flip(m) * width, LANES), width)

    def remote(src, dst, send, recv, ep_to, tp_to):
        return pltpu.make_async_remote_copy(
            src_ref=src, dst_ref=dst, send_sem=send, recv_sem=recv,
            device_id=(ep_to, tp_to), device_id_type=MESH,
        )

    evens = [6, 2, 4]
    half = size // 2
    odds = [m + 1 for m in evens] + [1]
    order = list(range(chunks))
    weights = [
        pltpu.make_async_copy(h.at[0], v, w_sem.at[i])
        for i, (h, v) in enumerate(((wg_hbm, wg), (wu_hbm, wu), (wd_hbm, wd)))
    ]
    for copy in weights:
        copy.start()

    spare = ep * tok_dev - count
    need = [min(tok_dev, -(-(-(-(size * (c + 1) + spare) // ep)) // 16) * 16) for c in order]
    need[-1] = tok_dev
    least = [size * c // ep // 16 * 16 for c in order]
    done = [min(tok_dev, size * (c + 1) // ep // 16 * 16) for c in order]
    done[-1] = tok_dev

    def piece(ends, c):
        start = ends[c - 1] if c else 0
        return pl.ds(start, ends[c] - start)

    barrier = pltpu.get_barrier_semaphore()
    for m in range(1, tp):
        pl.semaphore_signal(barrier, inc=1, device_id=(me, flip(m)), device_id_type=MESH)
    for k in range(1, ep):
        pl.semaphore_signal(
            barrier, inc=1, device_id=(lax.rem(me + k, ep), t), device_id_type=MESH
        )
    pl.semaphore_wait(barrier, tp + ep - 2)

    def z_copy(c, k):
        rows_c = piece(need, c)
        return remote(
            tok.at[rows_c, :], near.at[k, rows_c, :], z_send.at[c, k], z_recv.at[c, k],
            lax.rem(me + k, ep), t,
        )

    for c in order:
        if piece(need, c).size:
            for k in range(1, ep):
                z_copy(c, k).start()

    def gain_copy(m):
        return remote(
            gain, gain_all.at[:, cols(0)], g_send.at[m], g_recv.at[m], me, flip(m)
        )

    def gain_wait(m):
        remote(gain, gain_all.at[:, cols(m)], g_send.at[m], g_recv.at[m], me, flip(m)).wait_recv()

    for m in range(1, tp):
        gain_copy(m).start()
    gain_all[:, cols(0)] = gain[...]

    chosen_row[...] = jnp.full(chosen_row.shape, -1.0, f32)
    aff_row[...] = jnp.zeros(aff_row.shape, f32)
    chosen_row[:, :count] = chosen[...].astype(f32)
    aff_row[:, :count] = aff[...]
    diagonal = lax.broadcasted_iota(jnp.int32, (rows, rows), 0) == lax.broadcasted_iota(
        jnp.int32, (rows, rows), 1
    )
    given = jnp.sum(jnp.where(diagonal, chosen_row[...], 0.0), axis=1, keepdims=True)
    factor = jnp.sum(jnp.where(diagonal, aff_row[...], 0.0), axis=1, keepdims=True)

    owners = [lax.rem(me + q, ep) for q in range(ep)]
    lane = lax.broadcasted_iota(jnp.int32, (rows, tok_dev), 1)
    sub = lax.broadcasted_iota(jnp.int32, (tok_dev, rows), 0)
    taken_row, taken_col = [], []
    for q in range(ep):
        match = given == (lane + owners[q] * tok_dev).astype(f32)
        taken_row.append(jnp.sum(match.astype(f32), axis=0, keepdims=True))
        aff_token[q] = jnp.sum(jnp.where(match, factor, 0.0), axis=0, keepdims=True)
        match = chosen_row[...] == (sub + owners[q] * tok_dev).astype(f32)
        taken_col.append(jnp.sum(match.astype(f32), axis=1, keepdims=True))
    down_index = lax.broadcasted_iota(jnp.int32, (tok_dev, tok_dev), 0) * ep
    across_index = lax.broadcasted_iota(jnp.int32, (tok_dev, tok_dev), 1) * ep
    for q in range(ep):
        ahead = jnp.zeros((tok_dev, tok_dev), f32)
        above = jnp.zeros((tok_dev, tok_dev), f32)
        for p in range(ep):
            ahead = ahead + jnp.where(
                down_index + owners[p] < across_index + owners[q], taken_col[p], 0.0
            )
            above = above + jnp.where(
                across_index + owners[p] < down_index + owners[q], taken_row[p], 0.0
            )
        slot_row[q] = jnp.where(taken_row[q] > 0, jnp.sum(ahead, axis=0, keepdims=True), -1.0)
        slot_col[q] = jnp.where(taken_col[q] > 0, jnp.sum(above, axis=1, keepdims=True), -1.0)

    def span(c):
        return pl.ds(c * size, size)

    routes = {
        1: (0, None, 1), 2: (0, None, 2), 4: (0, None, 4),
        3: (2, None, 1), 6: (2, 0, 4), 5: (4, None, 1), 8: (4, 1, 2),
        7: (6, 0, 1), 9: (6, 1, 1),
    }

    def ag_block(c, m, part_of):
        if part_of is None:
            return full.at[flip(m), span(c), :]
        return full.at[flip(m), pl.ds(c * size + part_of * half, half), :]

    def ag_copy(c, s):
        m, part_of, to = routes[s]
        block = ag_block(c, m, part_of)
        return remote(block, block, ag_send.at[c, s], ag_recv.at[c, s], me, flip(to))

    def ag_wait(c, s):
        m, part_of, to = routes[s]
        block = ag_block(c, m ^ to, part_of)
        remote(block, block, ag_send.at[c, s], ag_recv.at[c, s], me, flip(to)).wait_recv()

    def pick(c):
        if piece(need, c).size:
            for k in range(1, ep):
                z_copy(c, k).wait_recv()
        low, high = least[c], need[c]
        place = (lax.broadcasted_iota(jnp.int32, (size, high - low), 0) + c * size).astype(f32)
        total = jnp.zeros((size, width), f32)
        scale = jnp.zeros((size, high - low), f32)
        for k in range(ep):
            q = (ep - k) % ep
            hot = (place == slot_row[q, :, low:high]).astype(f32)
            scale = scale + hot * aff_token[q, :, low:high]
            block = tok[low:high, :] if k == 0 else near[k, low:high, :]
            total = total + jnp.dot(hot.astype(bf16), block, preferred_element_type=f32)
        aff_col[span(c), :] = jnp.sum(scale, axis=1, keepdims=True)
        full[t, span(c), :] = total.astype(bf16)
        for s in (2, 4, 1):
            ag_copy(c, s).start()

    def forward(c, stages):
        for s, onward in stages:
            ag_wait(c, s)
            for after in onward:
                ag_copy(c, after).start()

    first = ((2, (6, 3)), (4, (8, 5)))
    second = ((6, (7,)), (8, (9,)))

    sums = (
        (2, 0, 0, 2), (4, 1, 0, 4), (6, 0, 1, 2), (6, 1, 1, 4), (4, 0, 2, 4), (2, 1, 2, 2),
    )

    def r2_copy(c, s):
        m, part_of, slot, to = sums[s]
        rows_h = pl.ds(part_of * half, half)
        return remote(
            part.at[c, m, rows_h, :], got2.at[c, slot, rows_h, :],
            r2_send.at[c, s], r2_recv.at[c, s], me, flip(to),
        )

    def relay(c):
        for s, m, part_of in ((2, 4, 0), (3, 2, 1)):
            rows_h = pl.ds(part_of * half, half)
            r2_copy(c, s).wait_recv()
            part[c, m, rows_h, :] = (
                keep[c, part_of] + got2[c, 1, rows_h, :].astype(f32)
            ).astype(bf16)
            r2_copy(c, s + 2).start()

    def finish(c):
        for s in (0, 1, 4, 5):
            r2_copy(c, s).wait_recv()
        total = own[span(c), :] + got2[c, 0].astype(f32) + got2[c, 2].astype(f32)
        weighted[span(c), :] = (total * aff_col[span(c), :]).astype(bf16)
        if piece(done, c).size:
            for k in list(range(1, ep)) + [0]:
                at_tokens(c, k)

    def at_tokens(c, k):
        rows_c, slots = piece(done, c), size * (c + 1)
        place = lax.broadcasted_iota(jnp.int32, (rows_c.size, slots), 1).astype(f32)
        hot = (slot_col[k, rows_c, :] == place).astype(f32).astype(bf16)
        back[k, rows_c, :] = jnp.dot(
            hot, weighted[:slots, :], preferred_element_type=f32
        ).astype(bf16)
        if k:
            back_copy(c, k).start()

    def back_copy(c, k):
        rows_c = piece(done, c)
        return remote(
            back.at[k, rows_c, :], got_back.at[k, rows_c, :], b_send.at[c, k], b_recv.at[c, k],
            lax.rem(me + k, ep), t,
        )

    tile = min(ff, 256)
    pick(0)
    for c in order[1:]:
        pick(c)
        if c == 1:
            forward(0, first)
            forward(1, first)
            forward(0, second)
    for m in range(1, tp):
        gain_wait(m)
    for position, c in enumerate(order):
        for s in (1, 3, 5, 7, 9):
            ag_wait(c, s)
        square_sum = jnp.zeros((size, 1), f32)
        for b in range(tp):
            floats = full[b, span(c), :].astype(f32)
            square_sum = square_sum + jnp.sum(floats * floats, axis=1, keepdims=True)
        scale = lax.rsqrt(square_sum / d + EPS)
        for b in range(tp):
            at = slice(b * width, (b + 1) * width)
            floats = full[b, span(c), :].astype(f32)
            normed[:, at] = (floats * scale * gain_all[:, at]).astype(bf16)
        if position == 0:
            weights[0].wait()
            weights[1].wait()

        @pl.loop(0, ff // tile)
        def _(j):
            units = pl.ds(pl.multiple_of(j * tile, LANES), tile)
            gate = jnp.dot(normed[...], wg[:, units], preferred_element_type=f32)
            upward = jnp.dot(normed[...], wu[:, units], preferred_element_type=f32)
            hidden[:, units] = (gate / (1.0 + jnp.exp(-gate)) * upward).astype(bf16)

        if position + 1 < chunks:
            if position + 2 < chunks:
                forward(position + 2, first)
            forward(position + 1, second)
        if position:
            relay(position - 1)
        if position == 0:
            weights[2].wait()

        def down(m):
            return jnp.dot(hidden[...], wd[:, cols(m)], preferred_element_type=f32)

        for m in odds:
            part[c, m] = down(m).astype(bf16)
            remote(
                part.at[c, m], got1.at[c, m - 1], r1_send.at[c, m], r1_recv.at[c, m - 1],
                me, flip(1),
            ).start()
        for m in evens + [0]:
            mine = down(m)
            remote(
                part.at[c, m + 1], got1.at[c, m], r1_send.at[c, m + 1], r1_recv.at[c, m],
                me, flip(1),
            ).wait_recv()
            mine = mine + got1[c, m].astype(f32)
            if m == 6:
                part[c, 6] = mine.astype(bf16)
                r2_copy(c, 2).start()
                r2_copy(c, 3).start()
            elif m:
                part_of = 0 if m == 2 else 1
                sent, kept = pl.ds(part_of * half, half), (1 - part_of) * half
                part[c, m, sent, :] = mine[part_of * half : part_of * half + half].astype(bf16)
                r2_copy(c, part_of).start()
                keep[c, 1 - part_of] = mine[kept : kept + half]
            else:
                own[span(c), :] = mine

        if position >= LAG:
            finish(position - LAG)
    relay(chunks - 1)
    for c in order[max(0, chunks - LAG):]:
        finish(c)

    for c in order:
        if piece(done, c).size:
            rows_c = piece(done, c)
            mix = back[0, rows_c, :].astype(f32)
            for k in range(1, ep):
                back_copy(c, k).wait_recv()
                mix = mix + got_back[k, rows_c, :].astype(f32)
            out[rows_c, :] = mix.astype(bf16)

    for m in range(1, tp):
        gain_copy(m).wait_send()
    for c in order:
        for k in range(1, ep):
            if piece(need, c).size:
                z_copy(c, k).wait_send()
            if piece(done, c).size:
                back_copy(c, k).wait_send()
        for s in routes:
            ag_copy(c, s).wait_send()
        for s in range(len(sums)):
            r2_copy(c, s).wait_send()
        for m in odds:
            remote(
                part.at[c, m], got1.at[c, m - 1], r1_send.at[c, m], r1_recv.at[c, m - 1],
                me, flip(1),
            ).wait_send()


def fused(ep, tp, tokens, norm_gain, chosen, affinity, w_gate, w_up, w_down):
    tok_dev, width = tokens.shape
    d, ff = w_gate.shape[1:]
    count = chosen.shape[1]
    step = 32 * CHUNKS
    rows = -(-count // step) * step
    size = rows // CHUNKS
    f32, bf16 = jnp.float32, jnp.bfloat16
    vmem = pl.BlockSpec(memory_space=pltpu.VMEM)
    hbm = pl.BlockSpec(memory_space=pl.ANY)
    dma = pltpu.SemaphoreType.DMA
    return pl.pallas_call(
        functools.partial(kernel, ep, tp, CHUNKS),
        out_shape=jax.ShapeDtypeStruct((tok_dev, width), bf16),
        in_specs=[vmem] * 4 + [hbm] * 3,
        out_specs=vmem,
        scratch_shapes=[
            pltpu.VMEM((d, ff), bf16),
            pltpu.VMEM((d, ff), bf16),
            pltpu.VMEM((ff, d), bf16),
            pltpu.VMEM((tp, rows, width), bf16),
            pltpu.VMEM((size, d), bf16),
            pltpu.VMEM((size, ff), bf16),
            pltpu.VMEM((CHUNKS, tp, size, width), bf16),
            pltpu.VMEM((CHUNKS, tp, size, width), bf16),
            pltpu.VMEM((CHUNKS, tp, size, width), bf16),
            pltpu.VMEM((rows, width), f32),
            pltpu.VMEM((rows, width), bf16),
            pltpu.VMEM((ep, tok_dev, width), bf16),
            pltpu.VMEM((ep, tok_dev, width), bf16),
            pltpu.VMEM((ep, tok_dev, width), bf16),
            pltpu.VMEM((1, rows), f32),
            pltpu.VMEM((1, rows), f32),
            pltpu.VMEM((ep, 1, tok_dev), f32),
            pltpu.VMEM((ep, 1, tok_dev), f32),
            pltpu.VMEM((ep, tok_dev, 1), f32),
            pltpu.VMEM((rows, 1), f32),
            pltpu.VMEM((1, d), f32),
            pltpu.VMEM((CHUNKS, 2, size // 2, width), f32),
            dma((3,)),
            dma((tp,)),
            dma((tp,)),
            dma((CHUNKS, ep)),
            dma((CHUNKS, ep)),
            dma((CHUNKS, 2 * tp)),
            dma((CHUNKS, 2 * tp)),
            dma((CHUNKS, tp)),
            dma((CHUNKS, tp)),
            dma((CHUNKS, tp)),
            dma((CHUNKS, tp)),
            dma((CHUNKS, ep)),
            dma((CHUNKS, ep)),
        ],
        compiler_params=pltpu.CompilerParams(
            collective_id=0, has_side_effects=True, vmem_limit_bytes=VMEM_BYTES
        ),
    )(tokens, norm_gain[None, :], chosen, affinity, w_gate, w_up, w_down)


EPS = 1e-06


def plain(tokens, norm_gain, chosen, affinity, w_gate, w_up, w_down):
    tok_dev, width_part = tokens.shape
    ep_count = lax.axis_size("ep")
    floats = tokens.astype(jnp.float32)
    square_sum = lax.psum(jnp.sum(floats * floats, axis=1), "tp")
    normed = (floats * lax.rsqrt(square_sum / w_gate.shape[1] + EPS)[:, None] * norm_gain[None, :]).astype(
        jnp.bfloat16
    )
    own_choice = chosen[0]
    chosen_count = own_choice.shape[0]
    bound_rows = min(tok_dev, 2 * chosen_count // ep_count)
    slot_ids = jnp.arange(bound_rows, dtype=jnp.int32)
    positions = jnp.arange(chosen_count, dtype=jnp.int32)
    every_token = lax.all_gather(normed, "ep", axis=0, tiled=True)
    picked = every_token[own_choice]
    piece = lax.all_gather(picked, "tp", axis=1, tiled=True)
    gate_rows = w_gate[0]
    up_rows = w_up[0]
    gate = jnp.dot(piece, gate_rows, preferred_element_type=jnp.float32)
    upward = jnp.dot(piece, up_rows, preferred_element_type=jnp.float32)
    hidden = (jax.nn.silu(gate) * upward).astype(jnp.bfloat16)
    columns = w_down[0]
    summed = lax.psum_scatter(
        lax.dot_general(
            columns, hidden, (((0,), (1,)), ((), ())), preferred_element_type=jnp.float32
        ).astype(jnp.bfloat16),
        "tp",
        scatter_dimension=0,
        tiled=True,
    ).astype(jnp.float32)
    weighted = (summed * affinity[0][None, :]).astype(jnp.bfloat16).T
    owner = own_choice // tok_dev
    owner_local = own_choice - owner * tok_dev
    owner_hot = owner[:, None] == jnp.arange(ep_count, dtype=jnp.int32)[None, :]
    running = jnp.cumsum(owner_hot.astype(jnp.int32), axis=0)
    place = jnp.sum(jnp.where(owner_hot, running, 0), axis=1) - 1
    back_match = owner_hot.T[:, None, :] & (place[None, None, :] == slot_ids[None, :, None])
    back_filled = jnp.any(back_match, axis=2)
    back_pick = jnp.sum(jnp.where(back_match, positions[None, None, :], 0), axis=2)
    back_rows = jnp.where(back_filled[..., None], weighted[back_pick], jnp.zeros((), jnp.bfloat16))
    back_token = jnp.where(back_filled, owner_local[back_pick], tok_dev)
    got_back, got_token = (
        lax.all_to_all(back_rows, "ep", split_axis=0, concat_axis=0, tiled=True),
        lax.all_to_all(back_token, "ep", split_axis=0, concat_axis=0, tiled=True),
    )
    total = jnp.zeros((tok_dev, width_part), jnp.float32)
    total = total.at[got_token.reshape(-1)].add(
        got_back.reshape(-1, width_part).astype(jnp.float32), mode="drop"
    )
    return total.astype(jnp.bfloat16)


def solution(mesh):
    ep, tp = mesh.shape["ep"], mesh.shape["tp"]

    def local(tokens, *rest):
        whole_lanes = tokens.shape[1] % LANES == 0 and rest[3].shape[2] % LANES == 0
        if whole_lanes and tp == 2**3:
            return fused(ep, tp, tokens, *rest)
        return plain(tokens, *rest)

    in_specs = (
        P("ep", "tp"),
        P("tp"),
        P("ep", None),
        P("ep", None),
        P("ep", None, "tp"),
        P("ep", None, "tp"),
        P("ep", "tp", None),
    )
    out_specs = P("ep", "tp")
    return jax.shard_map(local, mesh=mesh, in_specs=in_specs, out_specs=out_specs, check_vma=False)
```
